32 devices in a mesh: rep: 16 (over z, y, core), fs: 2 (over x), tp: 1.
Axes of the slice: x: 2, y: 2, z: 4, core: 2. Of those that a mesh axis runs over, the one named last changes fastest.
Arguments:
- pre_act: bfloat16 [16384, 4096], P('rep', ('fs', 'tp')), may hold values from -6 to 6
- down_weight: bfloat16 [4096, 2048], P(('fs', 'tp')), may hold values from -0.09375 to 0.09375
- cotangent: bfloat16 [16384, 2048], P('rep', ('fs', 'tp')), may hold values from -6 to 6
Outputs:
- grad_pre: bfloat16 [16384, 4096], P('rep', ('fs', 'tp'))
- grad_weight: float32 [4096, 2048], P(('fs', 'tp', 'rep'))
The draws below stay inside these ranges and needn't reach their ends.
All inputs are finite; a program needn't handle non-finite values.
Results may differ from the reference program's by a relative error of at most 0.0029.
Values may be sent and summed in bfloat16 or wider, within the bound.
A program may use at most 128 MiB of HBM per device.

```python
import jax
import jax.numpy as jnp

D = 2048
FF = 4096
TOKENS = 16384


def with_spikes(array, own_key, source, target, parts, factor):
    def block_of(position):
        return (jnp.arange(array.shape[position]) // (array.shape[position] // parts)).reshape((-1,) + (1,) * (array.ndim - 1 - position))

    first = jax.random.permutation(own_key, parts)[block_of(target)]
    other_side = (block_of(target) + parts // 2) % parts
    return jnp.where((block_of(source) == first) | (block_of(source) == other_side), factor * array, array)


def level_of(rng, dims, split, smallest, largest):
    factor_of = 1.0
    for axis_at, blocks in split:
        draws = jax.random.uniform(jax.random.fold_in(jax.random.fold_in(rng, 6), axis_at), (blocks,), jnp.float32, smallest / len(split), largest / len(split))
        factor_of = factor_of * jnp.repeat(jnp.exp(draws), dims[axis_at] // blocks).reshape((-1,) + (1,) * (len(dims) - 1 - axis_at))
    return factor_of


def bell_draw(key, extent, deviation, bound, cuts=(), kind=jnp.bfloat16):
    factor_of = level_of(key, extent, cuts, -0.22, 0.18) if cuts else 1.0
    drawn = jax.random.normal(key, extent, jnp.float32) * deviation * factor_of
    return jnp.minimum(jnp.maximum(drawn, -bound), bound).astype(kind)


def bell_draw_with(stream_key, dims, deviation, most, split, heavy, kind=jnp.bfloat16):
    entries = deviation * jax.random.normal(stream_key, dims, jnp.float32)
    if split:
        entries = entries * level_of(stream_key, dims, split, -0.22, 0.18)
    return jnp.clip(with_spikes(entries, jax.random.fold_in(stream_key, 3), *heavy), -most, most).astype(kind)


def setup_inputs(seed: int = 0) -> dict:
    arg_keys = jax.random.split(jax.random.key(seed), 4)
    pre_act = bell_draw(arg_keys[0], (TOKENS, FF), 1.0, 6.0, ((0, 16), (1, 2)))
    down_weight = bell_draw(arg_keys[1], (FF, D), FF ** -0.5, 0.09375, ((0, 2),))
    cotangent = bell_draw_with(arg_keys[2], (TOKENS, D), 1.0, 6.0, ((0, 16), (1, 2)), (0, 1, 16, 2.0))
    return {"pre_act": pre_act, "down_weight": down_weight, "cotangent": cotangent}


def reference(pre_act, down_weight, cotangent):
    grad_hidden = jnp.dot(cotangent, down_weight.T, preferred_element_type=jnp.float32)
    positive = jnp.maximum(pre_act.astype(jnp.float32), 0.0)
    grad_pre = (grad_hidden * 2.0 * positive).astype(jnp.bfloat16)
    hidden = (positive * positive).astype(jnp.bfloat16)
    summed = jnp.dot(hidden.T, cotangent, preferred_element_type=jnp.float32)
    grad_weight = summed * (1.0 / jnp.sqrt(jnp.float32(TOKENS)))
    return (grad_pre, grad_weight)
```

```python
import contextlib
import functools

import jax
import jax.numpy as jnp
from jax import lax
from jax.experimental import pallas as pl
from jax.experimental.pallas import tpu as pltpu
from jax.sharding import PartitionSpec as P

MESH = pl.DeviceIdType.MESH
CORES, ROWS = 2, 2
F32, BF16 = jnp.float32, jnp.bfloat16


NEAR, FAR = (4, 4, 4, 4), (4, 4, 2, 2, 2, 2)
CUTS = (2, 4)
FIRST_Z, RELAYS = 0, range(6)
ORDER = (
    "n0 n1 A1 o4",
    "n2 A0 n3 i4",
    "A3 g3 B0 g2",
    "B1 g1 x0 s1",
    "B3 f0 A4 t0",
    "B4 A2 B2 s3",
    "s4 x1 t3 f1",
    "t1 A5 t4 x2",
    "B5 h1 s2 f2",
    "h3 A6 v0 h2",
    "t2 x3 s5 f3",
    "A7 B7 l1 g0",
    "B6 l4 k3 s6",
    "x4 f4 A8 t5",
    "k2 l2 h0 x5",
    "f5 s7 l0 B8",
    "k0 x6 P9 f6",
    "A9 s8 k1 B9",
    "e2 e0 e1 s9.0",
    "e3 l6 l5 l3",
    "s9.1 s9.2 s9.3 l7",
    "l8 l9",
)


def scope(name):
    return contextlib.nullcontext()


def chunks_of(width, sizes):
    out, at = [], 0
    for s in sizes:
        out.append((at, s))
        at += s
    assert at == width
    return out


def plain(pre_act, down_weight, cotangent):
    whole = lax.all_gather(cotangent, ("fs", "tp"), axis=1, tiled=True)
    grad_hidden = lax.dot_general(
        whole, down_weight, (((1,), (1,)), ((), ())), preferred_element_type=F32
    )
    positive = jnp.maximum(pre_act.astype(F32), 0.0)
    grad_pre = (grad_hidden * 2.0 * positive).astype(BF16)
    hidden = (positive * positive).astype(BF16)
    factor = 1.0 / jnp.sqrt(jnp.float32(pre_act.shape[0] * lax.axis_size("rep")))
    term = lax.dot_general(
        hidden, whole, (((0,), (0,)), ((), ())), preferred_element_type=F32
    )
    summed = lax.psum_scatter(term, "rep", scatter_dimension=0, tiled=True)
    return (grad_pre, summed * factor)


def kernel(
    depth, near, far, crossing, marks, first_z, pieces, relays, order, factor,
    pre_hbm, w_hbm, cot_hbm, gp, gw,
    pre, pre_in, turned, w, cot, grad,
    y_out, y_in, own, z_out, z_in, b_sum, b_in, part,
    s_local, s_pre_s, s_pre_r, s_near_s, s_near_r, s_x_s, s_x_r, s_fwd_s, s_fwd_r,
    s_y_s, s_y_r, s_z_s, s_z_r, s_b_s, s_b_r,
):
    rep, fs, tp = lax.axis_index("rep"), lax.axis_index("fs"), lax.axis_index("tp")
    c, y, z = rep % CORES, (rep // CORES) % ROWS, rep // (CORES * ROWS)
    tokens, half = cot_hbm.shape
    hid = w_hbm.shape[0]
    block = own.shape[1]
    blocks = 2 * depth

    def at(z_, y_, c_, f_):
        return ((z_ * ROWS + y_) * CORES + c_, f_, tp)

    partner, across, beside = at(z, y, 1 - c, fs), at(z, y, c, 1 - fs), at(z, 1 - y, c, fs)

    def remote(src, dst, s, r, to):
        return pltpu.make_async_remote_copy(
            src_ref=src, dst_ref=dst, send_sem=s, recv_sem=r, device_id=to, device_id_type=MESH
        )

    def columns(i, c_):
        y_ = (1 - y) if i < depth else y
        k = (i % depth) * ROWS + y_
        return pl.ds(pl.multiple_of((k * CORES + c_) * block, block), block)

    def local(i, src, dst):
        return pltpu.make_async_copy(src, dst, s_local.at[i])

    loads = [local(0, pre_hbm, pre), local(1, cot_hbm, cot.at[0, pl.ds(0, tokens)]), local(2, w_hbm, w)]
    for l in loads:
        l.start()

    barrier = pltpu.get_barrier_semaphore()
    peers = [partner, across, beside]
    for d in range(1, depth):
        peers.append(at((z + d) % depth, y, c, fs))
    for p in peers:
        pl.semaphore_signal(barrier, inc=1, device_id=p, device_id_type=MESH)
    with scope("bar"):
        pl.semaphore_wait(barrier, len(peers))

    x_copies = []
    for q, (a, n, r, rn) in enumerate(crossing):
        x_copies.append(remote(
            cot_hbm.at[pl.ds(r, rn), pl.ds(a, n)], cot.at[1, pl.ds(r, rn), pl.ds(a, n)],
            s_x_s.at[q], s_x_r.at[q], across))
    x_copies[0].start()
    pre_copies = []
    for i in range(blocks):
        pre_copies.append(remote(
            pre_hbm.at[:, columns(i, 1 - c)], pre_in.at[i], s_pre_s.at[i], s_pre_r.at[i], partner))
    near_copies = []
    for q, (a, n) in enumerate(near):
        near_copies.append(remote(
            cot_hbm.at[:, pl.ds(a, n)], cot.at[0, pl.ds(tokens, tokens), pl.ds(a, n)],
            s_near_s.at[q], s_near_r.at[q], partner))
    for group in (pre_copies[:depth], near_copies[:2], pre_copies[depth:], near_copies[2:]):
        for copy in group:
            copy.start()
    for xc in x_copies[1:]:
        xc.start()

    def turn(v):
        p = jnp.maximum(v.astype(F32), 0.0)
        return (p * p).T.astype(BF16)

    strip = 256

    def turn_own(first):
        for i in range(first, first + depth):
            cols = columns(i, c)

            @pl.loop(0, tokens // strip, unroll=2)
            def _(t):
                rows = pl.ds(pl.multiple_of(t * strip, strip), strip)
                turned[pl.ds(i * block, block), rows] = turn(pre[rows, cols])

    def turn_in(first):
        for i in range(first, first + depth):
            pre_copies[i].wait_recv()

        @pl.loop(first, first + depth)
        def _(i):
            @pl.loop(0, tokens // strip, unroll=2)
            def _(t):
                rows = pl.ds(pl.multiple_of(t * strip, strip), strip)
                to = pl.ds(pl.multiple_of(tokens + t * strip, strip), strip)
                turned[pl.ds(pl.multiple_of(i * block, block), block), to] = turn(pre_in[i, rows, :])

    tall = 2 * block

    chunks = [(0, a, n) for a, n in near] + [(1, a, n) for a, n in far]

    def span(h, a, n):
        return pl.ds(h * half + a, n)

    def y_copy(j, p=0):
        h, a, n = chunks[j]
        s = span(h, a, n)
        if j == first_z:
            return remote(y_out.at[z, :, s], b_in, s_y_s.at[j], s_y_r.at[j], beside)
        each = depth // pieces[j]
        rows = pl.ds(p * each, each)
        return remote(
            y_out.at[rows, :, s], y_in.at[rows, :, s], s_y_s.at[j + p], s_y_r.at[j + p], beside)

    slots, far_end = depth, depth - 1
    inner = (z > 0) & (z < far_end)

    def relayed(j):
        return j in relays

    def z_block(j, kind):
        if kind == "up":
            ends = (z == far_end) if relayed(j) else False
            return jnp.where(ends, 0, (z + 1) % depth), jnp.where(ends, 3, 0), jnp.where(ends, far_end - 1, (z + 1) % depth)
        if kind == "down":
            ends = (z == 0) if relayed(j) else False
            return jnp.where(ends, far_end, (z + far_end) % depth), jnp.where(ends, 3, 2), jnp.where(ends, 1, (z + far_end) % depth)
        return (z + 2) % depth, 1, (z + 2) % depth

    def z_copy(j, kind, of_beside=False):
        h, a, n = chunks[j]
        s = span(h, a, n)
        block_, slot, to = z_block(j, kind)
        if of_beside:
            return remote(
                y_out.at[block_, :, s], y_in.at[slot, :, s], s_b_s.at[slot], s_b_r.at[slot], at(to, y, c, fs))
        return remote(
            z_out.at[block_, :, s], z_in.at[slot, :, s],
            s_z_s.at[j * slots + slot], s_z_r.at[j * slots + slot], at(to, y, c, fs))

    def z_arrival(j, slot, of_beside=False):
        h, a, n = chunks[j]
        s = span(h, a, n)
        if of_beside:
            return remote(y_out.at[0, :, s], y_in.at[slot, :, s], s_b_s.at[slot], s_b_r.at[slot], beside)
        return remote(
            z_out.at[0, :, s], z_in.at[slot, :, s],
            s_z_s.at[j * slots + slot], s_z_r.at[j * slots + slot], beside)

    def z_send(j, of_beside=False):
        z_copy(j, "up", of_beside).start()
        z_copy(j, "down", of_beside).start()
        if relayed(j):

            @pl.when(jnp.logical_not(inner))
            def _():
                z_copy(j, "two", of_beside).start()
        else:
            z_copy(j, "two", of_beside).start()

    def fwd_copy(q):
        a, n, r, rn = crossing[q]
        return remote(
            cot.at[1, pl.ds(r, rn), pl.ds(a, n)], cot.at[1, pl.ds(tokens + r, rn), pl.ds(a, n)],
            s_fwd_s.at[q], s_fwd_r.at[q], partner)

    def dot(j, m, which=None):
        h, a, n = chunks[j]
        rows = pl.ds(pl.multiple_of(m * tall, tall), tall)
        if which is None:
            return lax.dot_general(
                turned[rows, :], cot[h, :, pl.ds(a, n)], (((1,), (0,)), ((), ())),
                preferred_element_type=F32).reshape(2, block, n)
        r, rn = crossing[which][2:]

        def over(first):
            ts = pl.ds(first + r, rn)
            return lax.dot_general(
                turned[rows, ts], cot[h, ts, pl.ds(a, n)], (((1,), (0,)), ((), ())),
                preferred_element_type=F32)

        return (over(0) + over(tokens)).reshape(2, block, n)

    def product_start(j):
        h, a, n = chunks[j]
        s = span(h, a, n)
        for m in range(depth // 2):
            part[pl.ds(m * 2, 2)] = dot(j, m, -2)
            own[pl.ds(m * 2, 2), :, s] = dot(j, m + depth // 2, -2)

    def product_beside(j):
        h, a, n = chunks[j]
        s = span(h, a, n)
        if pieces[j] > 1:
            for m in range(depth // 2):
                y_out[pl.ds(m * 2, 2), :, s] = (part[pl.ds(m * 2, 2)] + dot(j, m, -1)).astype(BF16)
                y_copy(j, 2 * m).start()
                y_copy(j, 2 * m + 1).start()
            return

        @pl.loop(0, depth // 2, unroll=True)
        def _(m):
            y_out[pl.ds(m * 2, 2), :, s] = dot(j, m).astype(BF16)

        if j == first_z:
            b_sum[...] = y_out[z, :, s].astype(F32)
            z_send(j, True)
        else:
            y_copy(j).start()

    def product_own(j):
        h, a, n = chunks[j]
        s = span(h, a, n)
        if pieces[j] > 1:
            for m in range(depth // 2):
                own[pl.ds(m * 2, 2), :, s] += dot(j, m + depth // 2, -1)
            return

        @pl.loop(0, depth // 2, unroll=True)
        def _(m):
            v = dot(j, m + depth // 2)
            own[pl.ds(m * 2, 2), :, s] = v
            if j == first_z:
                z_out[pl.ds(m * 2, 2), :, s] = v.astype(BF16)

        if j == first_z:
            z_send(j)

    def second(j, p=0):
        h, a, n = chunks[j]
        s = span(h, a, n)
        each = depth // pieces[j]
        with scope(f"wy{j}"):
            y_copy(j, p).wait_recv()

        @pl.loop(p * each, (p + 1) * each, unroll=each < depth)
        def _(k):
            v = own[k, :, s] + y_in[k, :, s].astype(F32)
            own[k, :, s] = v
            z_out[k, :, s] = v.astype(BF16)

        if pieces[j] == 1:
            z_send(j)
            return
        for kind in ("up", "down", "two"):

            @pl.when(z_block(j, kind)[0] // each == p)
            def _(kind=kind):
                z_copy(j, kind).start()

    def third(j):
        h, a, n = chunks[j]
        s = span(h, a, n)

        @pl.when(inner)
        def _():
            to = (z + 2) % depth
            with scope(f"wr{j}"):
                z_arrival(j, 3).wait_recv()
            z_out[to, :, s] = (own[to, :, s] + z_in[3, :, s].astype(F32)).astype(BF16)
            z_copy(j, "two").start()
            if j == first_z:
                z_arrival(j, 3, True).wait_recv()
                y_out[to, :, s] = (y_out[to, :, s].astype(F32) + y_in[3, :, s].astype(F32)).astype(BF16)
                z_copy(j, "two", True).start()

    def arrivals(j, add):
        for slot, there in ((0, z > 0), (2, z < far_end), (1, None)) if relayed(j) else ((0, None), (2, None), (1, None)):
            if there is None:
                add(slot)
            else:
                pl.when(there)(functools.partial(add, slot))

    def across_z(j):
        h, a, n = chunks[j]
        s = span(h, a, n)

        def add(slot):
            with scope(f"wb{j}s{slot}"):
                z_arrival(j, slot, True).wait_recv()
            b_sum[...] += y_in[slot, :, s].astype(F32)

        arrivals(j, add)
        y_out[z, :, s] = b_sum[...].astype(BF16)
        y_copy(j).start()

    def last(j):
        h, a, n = chunks[j]
        s = span(h, a, n)

        def add(slot):
            with scope(f"wz{j}s{slot}"):
                z_arrival(j, slot).wait_recv()
            own[z, :, s] = own[z, :, s] + z_in[slot, :, s].astype(F32)

        arrivals(j, add)
        place = pl.multiple_of((fs if h == 0 else 1 - fs) * half + a, 128)
        total_ = own[z, :, s]
        if j == first_z:
            y_copy(j).wait_recv()
            total_ = total_ + b_in[...].astype(F32)
        gw[:, pl.ds(place, n)] = total_ * factor

    tm, tn = 256, 512

    def grad_tile(h, a, n, m, k):
        rows = pl.ds(pl.multiple_of(m * tm, tm), tm)
        outs = pl.ds(pl.multiple_of(k * tn, tn), tn)
        place = pl.multiple_of((fs if h == 0 else 1 - fs) * half + a, 128)
        return rows, outs, lax.dot_general(
            cot[h, rows, pl.ds(a, n)], w[outs, pl.ds(place, n)], (((1,), (1,)), ((), ())),
            preferred_element_type=F32)

    weights = [loads[2]]

    def grad_first(m):
        if weights:
            weights.pop().wait()

        @pl.loop(0, hid // tn, unroll=True)
        def _(k):
            rows, outs, v = grad_tile(0, 0, half, m, k)
            grad[rows, outs] = v

    def grad_next(m, part):
        @pl.loop(0, hid // tn, unroll=True)
        def _(k):
            rows, outs, v = grad_tile(1, marks[part], marks[part + 1] - marks[part], m, k)
            grad[rows, outs] += v

    def grad_rest(m):
        @pl.loop(0, hid // tn, unroll=True)
        def _(k):
            rows, outs, v = grad_tile(1, marks[-2], marks[-1] - marks[-2], m, k)
            p = jnp.maximum(pre[rows, outs].astype(F32), 0.0)
            gp[rows, outs] = ((grad[rows, outs] + v) * 2.0 * p).astype(BF16)

    def near_in(q):
        near_copies[q].wait_recv()

    def far_in(q):
        x_copies[q].wait_recv()
        fwd_copy(q).start()

    def far_both(q):
        fwd_copy(q).wait_recv()

    nn, nf = len(near), len(far)
    total = nn + nf
    steps = {
        "A": product_beside, "B": product_own, "P": product_start,
        "s": second, "t": third, "v": across_z, "l": last, "n": near_in, "x": far_in, "f": far_both,
        "g": grad_first, "h": lambda m: grad_next(m, 0), "k": lambda m: grad_next(m, 1), "e": grad_rest,
        "o": turn_own, "i": turn_in,
    }
    with scope("ld0"):
        loads[0].wait()
    with scope("o0"):
        turn_own(0)
    loads[1].wait()
    with scope("i0"):
        turn_in(0)
    for step in " ".join(order).split():
        with scope(step):
            steps[step[0]](*(int(v) for v in step[1:].split(".")))

    with scope("drain"):
        for copy in pre_copies + near_copies + x_copies:
            copy.wait_send()
        for q in range(len(crossing)):
            fwd_copy(q).wait_send()
        for j in range(total):
            for p in range(pieces[j]):
                y_copy(j, p).wait_send()
            for kind in ("up", "down", "two"):
                z_copy(j, kind).wait_send()
                if j == first_z:
                    z_copy(j, kind, True).wait_send()


def solution(mesh):
    reps, fs, tp = mesh.shape["rep"], mesh.shape["fs"], mesh.shape["tp"]
    depth = reps // (CORES * ROWS)

    def on_device(pre_act, down_weight, cotangent):
        tokens, hid = pre_act.shape
        half = cotangent.shape[1]
        width = down_weight.shape[1]
        block = hid // reps
        if not (fs == 2 and tp == 1 and depth * CORES * ROWS == reps and depth == 4
                and block % 128 == 0 and half % 1024 == 0 and hid % 512 == 0 and tokens == 1024):
            return plain(pre_act, down_weight, cotangent)
        step = half // 4
        near = chunks_of(half, [step // 4 * v for v in NEAR])
        far = chunks_of(half, [step // 4 * v for v in FAR])
        nn, nf = len(near), len(far)
        total = nn + nf
        marks = [0] + [far[i][0] for i in CUTS] + [half]
        crossing = [(a, n, 0, tokens) for a, n in far]
        a, n = far[-1]
        crossing[-1:] = [(a, n, 0, tokens // 2), (a, n, tokens // 2, tokens // 2)]
        nx = len(crossing)
        pieces = [1] * (total - 1) + [depth]
        first_z, relays = FIRST_Z, RELAYS
        factor = 1.0 / float(tokens * reps) ** 0.5
        dma = lambda n: pltpu.SemaphoreType.DMA((n,))
        vm = pltpu.VMEM
        return pl.pallas_call(
            functools.partial(kernel, depth, near, far, crossing, marks, first_z, pieces, relays, ORDER, factor),
            out_shape=[
                pltpu.VMEM((tokens, hid), BF16),
                pltpu.VMEM((block, width), F32),
            ],
            in_specs=[pl.BlockSpec(memory_space=pl.ANY)] * 3,
            out_specs=[pl.BlockSpec(memory_space=pltpu.VMEM)] * 2,
            scratch_shapes=[
                vm((tokens, hid), BF16),
                vm((2 * depth, tokens, block), BF16),
                vm((2 * depth * block, 2 * tokens), BF16),
                vm(down_weight.shape, BF16),
                vm((2, 2 * tokens, half), BF16),
                vm((tokens, hid), F32),
                vm((depth, block, width), BF16),
                vm((depth, block, width), BF16),
                vm((depth, block, width), F32),
                vm((depth, block, width), BF16),
                vm((depth, block, width), BF16),
                vm((block, near[0][1]), F32),
                vm((block, near[0][1]), BF16),
                vm((depth, block, far[-1][1]), F32),
                dma(4), dma(2 * depth), dma(2 * depth), dma(nn), dma(nn), dma(nx), dma(nx), dma(nx), dma(nx),
                dma(total + depth), dma(total + depth), dma(total * depth), dma(total * depth), dma(depth), dma(depth),
            ],
            compiler_params=pltpu.CompilerParams(
                collective_id=0, has_side_effects=True, vmem_limit_bytes=56 * 1024 * 1024
            ),
            cost_estimate=pl.CostEstimate(
                flops=8 * tokens * hid * width // 2, bytes_accessed=40 * 1024 * 1024, transcendentals=0),
        )(pre_act, down_weight, cotangent)

    return jax.shard_map(
        on_device,
        mesh=mesh,
        in_specs=(P("rep", ("fs", "tp")), P(("fs", "tp"), None), P("rep", ("fs", "tp"))),
        out_specs=(P("rep", ("fs", "tp")), P(("fs", "tp", "rep"), None)),
        check_vma=False,
    )
```

```python
import contextlib
import functools

import jax
import jax.numpy as jnp
from jax import lax
from jax.experimental import pallas as pl
from jax.experimental.pallas import tpu as pltpu
from jax.sharding import PartitionSpec as P

MESH = pl.DeviceIdType.MESH
CORES, ROWS = 2, 2
F32, BF16 = jnp.float32, jnp.bfloat16


NEAR, FAR = (4, 4, 4, 4), (4, 4, 2, 2, 2, 2)
CUTS = (2, 4)
FIRST_Z, RELAYS = 0, range(6)
ORDER = (
    "n0 o4 n1 A1",
    "i4 n2 A0 n3",
    "A3 B3 B1 B0",
    "g3 g0 x0 s1",
    "g2 f0 A4 A2",
    "B2 s3 t0 B4",
    "t3 g1 x1 s4",
    "t1 f1 A5 B5",
    "h0 h1 h2 h3",
    "s2 t4 x2 v0",
    "f2 A6 B6 s5",
    "t2 x3 f3 A7",
    "B7 k0 k1 t5",
    "s6 k2 k3 x4",
    "f4 A8 B8 x5",
    "s7 x6 f5 P9",
    "f6 A9 s8.0 B9",
    "s8.1 e0 s8.2 s8.3",
    "e1 s9.0 l6 s9.1",
    "s9.2 l7 s9.3 e2",
    "e3 L0 l8 l9",
)


def scope(name):
    return contextlib.nullcontext()


def chunks_of(width, sizes):
    out, at = [], 0
    for s in sizes:
        out.append((at, s))
        at += s
    assert at == width
    return out


def plain(pre_act, down_weight, cotangent):
    whole = lax.all_gather(cotangent, ("fs", "tp"), axis=1, tiled=True)
    grad_hidden = lax.dot_general(
        whole, down_weight, (((1,), (1,)), ((), ())), preferred_element_type=F32
    )
    positive = jnp.maximum(pre_act.astype(F32), 0.0)
    grad_pre = (grad_hidden * 2.0 * positive).astype(BF16)
    hidden = (positive * positive).astype(BF16)
    factor = 1.0 / jnp.sqrt(jnp.float32(pre_act.shape[0] * lax.axis_size("rep")))
    term = lax.dot_general(
        hidden, whole, (((0,), (0,)), ((), ())), preferred_element_type=F32
    )
    summed = lax.psum_scatter(term, "rep", scatter_dimension=0, tiled=True)
    return (grad_pre, summed * factor)


def kernel(
    depth, near, far, crossing, marks, first_z, pieces, relays, order, factor,
    pre_hbm, w_hbm, cot_hbm, gp, gw,
    pre, pre_in, turned, w, cot, grad,
    y_out, y_in, own, z_out, z_in, b_sum, b_in, part,
    s_above, s_local, s_sent, s_pre_r, s_near_r, s_x_r, s_fwd_r, s_y_r, s_z_r, s_b_r,
):
    rep, fs, tp = lax.axis_index("rep"), lax.axis_index("fs"), lax.axis_index("tp")
    c, y, z = rep % CORES, (rep // CORES) % ROWS, rep // (CORES * ROWS)
    tokens, half = cot_hbm.shape
    hid = w_hbm.shape[0]
    block = own.shape[1]
    blocks = 2 * depth

    def at(z_, y_, c_, f_):
        return ((z_ * ROWS + y_) * CORES + c_, f_, tp)

    partner, across, beside = at(z, y, 1 - c, fs), at(z, y, c, 1 - fs), at(z, 1 - y, c, fs)

    def remote(src, dst, s, r, to):
        return pltpu.make_async_remote_copy(
            src_ref=src, dst_ref=dst, send_sem=s, recv_sem=r, device_id=to, device_id_type=MESH
        )

    def columns(i, c_):
        y_ = (1 - y) if i < depth else y
        k = (i % depth) * ROWS + y_
        return pl.ds(pl.multiple_of((k * CORES + c_) * block, block), block)

    def local(i, src, dst):
        return pltpu.make_async_copy(src, dst, s_local.at[i])

    loads = [local(0, cot_hbm, cot.at[0, pl.ds(0, tokens)]), local(1, pre_hbm, pre), local(2, w_hbm, w)]
    for l in loads:
        l.start()

    barrier = pltpu.get_barrier_semaphore()
    for p in (partner, across, beside):
        pl.semaphore_signal(barrier, inc=1, device_id=p, device_id_type=MESH)
    for d in range(1, depth):

        @pl.when(z + d < depth)
        def _(d=d):
            pl.semaphore_signal(barrier, inc=1, device_id=at(z + d, y, c, fs), device_id_type=MESH)

    with scope("bar"):
        pl.semaphore_wait(barrier, 3 + z)
    for d in range(1, depth):

        @pl.when(z >= d)
        def _(d=d):
            pl.semaphore_signal(s_above, inc=1, device_id=at(z - d, y, c, fs), device_id_type=MESH)

    x_copies = []
    for q, (a, n, r, rn) in enumerate(crossing):
        x_copies.append(remote(
            cot.at[0, pl.ds(r, rn), pl.ds(a, n)], cot.at[1, pl.ds(r, rn), pl.ds(a, n)],
            s_sent.at[2], s_x_r.at[q], across))
    pre_copies = []
    for i in range(blocks):
        pre_copies.append(remote(
            pre.at[:, columns(i, 1 - c)], pre_in.at[i], s_sent.at[0], s_pre_r.at[i // depth], partner))
    near_copies = []
    for q, (a, n) in enumerate(near):
        near_copies.append(remote(
            cot.at[0, pl.ds(0, tokens), pl.ds(a, n)], cot.at[0, pl.ds(tokens, tokens), pl.ds(a, n)],
            s_sent.at[1], s_near_r.at[q], partner))
    with scope("ld"):
        loads[0].wait()
    for xc in x_copies:
        xc.start()
    loads[1].wait()
    for group in (pre_copies[:depth], near_copies[:2], pre_copies[depth:], near_copies[2:]):
        for copy in group:
            copy.start()
    def turn(v):
        p = jnp.maximum(v.astype(F32), 0.0)
        return (p * p).T.astype(BF16)

    strip = 256

    def turn_own(first):
        for i in range(first, first + depth):
            cols = columns(i, c)

            @pl.loop(0, tokens // strip, unroll=2)
            def _(t):
                rows = pl.ds(pl.multiple_of(t * strip, strip), strip)
                turned[pl.ds(i * block, block), rows] = turn(pre[rows, cols])

    def turn_in(first):
        both = pre_in.at[pl.ds(first, depth)]
        remote(both, both, s_sent.at[0], s_pre_r.at[first // depth], partner).wait_recv()

        @pl.loop(first, first + depth)
        def _(i):
            @pl.loop(0, tokens // strip, unroll=2)
            def _(t):
                rows = pl.ds(pl.multiple_of(t * strip, strip), strip)
                to = pl.ds(pl.multiple_of(tokens + t * strip, strip), strip)
                turned[pl.ds(pl.multiple_of(i * block, block), block), to] = turn(pre_in[i, rows, :])

    tall = 2 * block

    chunks = [(0, a, n) for a, n in near] + [(1, a, n) for a, n in far]

    final = len(chunks) - 1

    def span(h, a, n):
        return pl.ds(h * half + a, n)

    def turn_of(p):
        return jnp.where(c == 0, p, p + 1 - 2 * (p % 2))

    def y_copy(j, p=0):
        h, a, n = chunks[j]
        s = span(h, a, n)
        if j == first_z:
            return remote(y_out.at[z, :, s], b_in, s_sent.at[5], s_y_r.at[sum(pieces[:j])], beside)
        rows = pl.ds(turn_of(p), 1) if pieces[j] > 1 else pl.ds(0, depth)
        return remote(
            y_out.at[rows, :, s], y_in.at[rows, :, s], s_sent.at[4], s_y_r.at[sum(pieces[:j]) + p], beside)

    slots, far_end = depth, depth - 1
    inner = (z > 0) & (z < far_end)

    def relayed(j):
        return j in relays

    def z_block(j, kind):
        if kind == "up":
            ends = (z == far_end) if relayed(j) else False
            return jnp.where(ends, 0, (z + 1) % depth), jnp.where(ends, 3, 0), jnp.where(ends, far_end - 1, (z + 1) % depth)
        if kind == "down":
            ends = (z == 0) if relayed(j) else False
            return jnp.where(ends, far_end, (z + far_end) % depth), jnp.where(ends, 3, 2), jnp.where(ends, 1, (z + far_end) % depth)
        return (z + 2) % depth, 1, (z + 2) % depth

    def z_copy(j, kind, of_beside=False):
        h, a, n = chunks[j]
        s = span(h, a, n)
        block_, slot, to = z_block(j, kind)
        relay = jnp.where(slot == 3, 1, 0)
        if of_beside:
            return remote(
                y_out.at[block_, :, s], y_in.at[slot, :, s], s_sent.at[7], s_b_r.at[relay], at(to, y, c, fs))
        return remote(
            z_out.at[block_, :, s], z_in.at[slot, :, s],
            s_sent.at[6], s_z_r.at[relay * (1 + j) if relayed(j) else 1 + j], at(to, y, c, fs))

    def arrived(ref, sem):
        remote(ref, ref, s_sent.at[6], sem, beside).wait_recv()

    def all_arrived(ref, cols, sem):
        pl.when(inner)(lambda: arrived(ref.at[pl.ds(0, 3), :, cols], sem))
        pl.when(jnp.logical_not(inner))(lambda: arrived(ref.at[pl.ds(0, 2), :, cols], sem))

    def z_send(j, of_beside=False):
        z_copy(j, "up", of_beside).start()
        z_copy(j, "down", of_beside).start()
        if relayed(j):

            @pl.when(jnp.logical_not(inner))
            def _():
                z_copy(j, "two", of_beside).start()
        else:
            z_copy(j, "two", of_beside).start()

    def fwd_copy(q):
        a, n, r, rn = crossing[q]
        return remote(
            cot.at[1, pl.ds(r, rn), pl.ds(a, n)], cot.at[1, pl.ds(tokens + r, rn), pl.ds(a, n)],
            s_sent.at[3], s_fwd_r.at[q], partner)

    def dot(j, m, which=None):
        h, a, n = chunks[j]
        rows = pl.ds(pl.multiple_of(m * tall, tall), tall)
        if which is None:
            return lax.dot_general(
                turned[rows, :], cot[h, :, pl.ds(a, n)], (((1,), (0,)), ((), ())),
                preferred_element_type=F32).reshape(2, block, n)
        r, rn = crossing[which][2:]

        def over(first):
            ts = pl.ds(first + r, rn)
            return lax.dot_general(
                turned[rows, ts], cot[h, ts, pl.ds(a, n)], (((1,), (0,)), ((), ())),
                preferred_element_type=F32)

        return (over(0) + over(tokens)).reshape(2, block, n)

    def product_start(j):
        h, a, n = chunks[j]
        s = span(h, a, n)
        for m in range(depth // 2):
            part[pl.ds(m * 2, 2)] = dot(j, m, -2)
            own[pl.ds(m * 2, 2), :, s] = dot(j, m + depth // 2, -2)

    def product_beside(j):
        h, a, n = chunks[j]
        s = span(h, a, n)
        if pieces[j] > 1:
            for m in range(depth // 2):
                v = part[pl.ds(m * 2, 2)] + dot(j, m, -1) if j == final else dot(j, m)
                y_out[pl.ds(m * 2, 2), :, s] = v.astype(BF16)
                y_copy(j, 2 * m).start()
                y_copy(j, 2 * m + 1).start()
            return

        @pl.loop(0, depth // 2, unroll=True)
        def _(m):
            y_out[pl.ds(m * 2, 2), :, s] = dot(j, m).astype(BF16)

        if j == first_z:
            b_sum[...] = y_out[z, :, s].astype(F32)
            z_send(j, True)
        else:
            y_copy(j).start()

    def product_own(j):
        h, a, n = chunks[j]
        s = span(h, a, n)
        if j == final:
            for m in range(depth // 2):
                own[pl.ds(m * 2, 2), :, s] += dot(j, m + depth // 2, -1)
            return

        @pl.loop(0, depth // 2, unroll=True)
        def _(m):
            v = dot(j, m + depth // 2)
            own[pl.ds(m * 2, 2), :, s] = v
            if j == first_z:
                z_out[pl.ds(m * 2, 2), :, s] = v.astype(BF16)

        if j == first_z:
            z_send(j)

    def second(j, p=0):
        h, a, n = chunks[j]
        s = span(h, a, n)
        with scope(f"wy{j}"):
            y_copy(j, p).wait_recv()

        def add(k):
            v = own[k, :, s] + y_in[k, :, s].astype(F32)
            own[k, :, s] = v
            z_out[k, :, s] = v.astype(BF16)

        if pieces[j] == 1:
            pl.loop(0, depth)(add)
            z_send(j)
            return
        k = turn_of(p)
        add(k)
        for kind in ("up", "down", "two"):

            @pl.when(z_block(j, kind)[0] == k)
            def _(kind=kind):
                z_copy(j, kind).start()

    def third(j):
        h, a, n = chunks[j]
        s = span(h, a, n)

        @pl.when(inner)
        def _():
            to = (z + 2) % depth
            with scope(f"wr{j}"):
                arrived(z_in.at[3, :, s], s_z_r.at[1 + j])
            z_out[to, :, s] = (own[to, :, s] + z_in[3, :, s].astype(F32)).astype(BF16)
            z_copy(j, "two").start()
            if j == first_z:
                arrived(y_in.at[3, :, s], s_b_r.at[1])
                y_out[to, :, s] = (y_out[to, :, s].astype(F32) + y_in[3, :, s].astype(F32)).astype(BF16)
                z_copy(j, "two", True).start()

    def arrivals(j, add):
        for slot, there in ((0, z > 0), (2, z < far_end), (1, None)) if relayed(j) else ((0, None), (2, None), (1, None)):
            if there is None:
                add(slot)
            else:
                pl.when(there)(functools.partial(add, slot))

    def across_z(j):
        h, a, n = chunks[j]
        s = span(h, a, n)
        with scope("wb"):
            all_arrived(y_in, s, s_b_r.at[0])

        def add(slot):
            b_sum[...] += y_in[slot, :, s].astype(F32)

        arrivals(j, add)
        y_out[z, :, s] = b_sum[...].astype(BF16)
        y_copy(j).start()

    def total_of(j):
        h, a, n = chunks[j]
        s = span(h, a, n)

        def add(slot):
            own[z, :, s] = own[z, :, s] + z_in[slot, :, s].astype(F32)

        arrivals(j, add)
        place = pl.multiple_of((fs if h == 0 else 1 - fs) * half + a, 128)
        v = own[z, :, s]
        if j == first_z:
            v = v + b_in[...].astype(F32)
        gw[:, pl.ds(place, n)] = v * factor

    def last(j):
        h, a, n = chunks[j]
        with scope(f"wz{j}"):
            arrived(z_in.at[pl.ds(0, 3), :, span(h, a, n)], s_z_r.at[1 + j])
        total_of(j)

    def last_relayed(_):
        h, a, n = chunks[len(relays) - 1]
        with scope("wL"):
            all_arrived(z_in, pl.ds(0, h * half + a + n), s_z_r.at[0])
        with scope("wLy"):
            if first_z is not None:
                y_copy(first_z).wait_recv()
        for j in relays:
            total_of(j)

    tm, tn = 256, 512

    def grad_tile(h, a, n, m, k):
        rows = pl.ds(pl.multiple_of(m * tm, tm), tm)
        outs = pl.ds(pl.multiple_of(k * tn, tn), tn)
        place = pl.multiple_of((fs if h == 0 else 1 - fs) * half + a, 128)
        return rows, outs, lax.dot_general(
            cot[h, rows, pl.ds(a, n)], w[outs, pl.ds(place, n)], (((1,), (1,)), ((), ())),
            preferred_element_type=F32)

    weights = [loads[2]]

    def grad_first(m):
        if weights:
            weights.pop().wait()

        @pl.loop(0, hid // tn, unroll=True)
        def _(k):
            rows, outs, v = grad_tile(0, 0, half, m, k)
            grad[rows, outs] = v

    def grad_next(m, part):
        @pl.loop(0, hid // tn, unroll=True)
        def _(k):
            rows, outs, v = grad_tile(1, marks[part], marks[part + 1] - marks[part], m, k)
            grad[rows, outs] += v

    def grad_rest(m):
        @pl.loop(0, hid // tn, unroll=True)
        def _(k):
            rows, outs, v = grad_tile(1, marks[-2], marks[-1] - marks[-2], m, k)
            p = jnp.maximum(pre[rows, outs].astype(F32), 0.0)
            gp[rows, outs] = ((grad[rows, outs] + v) * 2.0 * p).astype(BF16)

    def near_in(q):
        near_copies[q].wait_recv()

    def far_in(q):
        x_copies[q].wait_recv()
        fwd_copy(q).start()

    def far_both(q):
        fwd_copy(q).wait_recv()

    nn, nf = len(near), len(far)
    total = nn + nf
    steps = {
        "A": product_beside, "B": product_own, "P": product_start,
        "s": second, "t": third, "v": across_z, "l": last, "L": last_relayed, "n": near_in, "x": far_in, "f": far_both,
        "g": grad_first, "h": lambda m: grad_next(m, 0), "k": lambda m: grad_next(m, 1), "e": grad_rest,
        "o": turn_own, "i": turn_in,
    }
    with scope("o0"):
        turn_own(0)
    with scope("i0"):
        turn_in(0)
    with scope("above"):
        pl.when(z < depth - 1)(lambda: pl.semaphore_wait(s_above, depth - 1 - z))
    for step in " ".join(order).split():
        with scope(step):
            steps[step[0]](*(int(v) for v in step[1:].split(".")))

    with scope("drain"):
        skip = 0 if first_z is None else near[0][1]
        whole = cot.at[0, pl.ds(0, tokens)]
        first = pl.ds(0, skip)
        sent = [
            pre.at[:, pl.ds(0, blocks * block)], whole, whole, whole,
            y_out.at[:, :, pl.ds(skip, 2 * half - skip)], y_out.at[0, :, first],
            z_out.at[pl.ds(0, 3)], y_out.at[pl.ds(0, 3), :, first],
        ]
        for i, ref in enumerate(sent):
            if skip or i not in (5, 7):
                remote(ref, ref, s_sent.at[i], s_b_r.at[0], partner).wait_send()


PARTS = 4


def store(gp_in, gw_in, gp_out, gw_out, sems):
    rows = gp_in.shape[0] // PARTS
    copies = [pltpu.make_async_copy(gw_in, gw_out, sems.at[PARTS])]
    for i in range(PARTS):
        r = pl.ds(i * rows, rows)
        copies.append(pltpu.make_async_copy(gp_in.at[r], gp_out.at[r], sems.at[i]))
    for copy in copies:
        copy.start()
    for copy in copies:
        copy.wait()


def solution(mesh):
    reps, fs, tp = mesh.shape["rep"], mesh.shape["fs"], mesh.shape["tp"]
    depth = reps // (CORES * ROWS)

    def on_device(pre_act, down_weight, cotangent):
        tokens, hid = pre_act.shape
        half = cotangent.shape[1]
        width = down_weight.shape[1]
        block = hid // reps
        if not (fs == 2 and tp == 1 and depth * CORES * ROWS == reps and depth == 4
                and block % 128 == 0 and half % 1024 == 0 and hid % 512 == 0 and tokens == 1024):
            return plain(pre_act, down_weight, cotangent)
        step = half // 4
        near = chunks_of(half, [step // 4 * v for v in NEAR])
        far = chunks_of(half, [step // 4 * v for v in FAR])
        nn, nf = len(near), len(far)
        total = nn + nf
        marks = [0] + [far[i][0] for i in CUTS] + [half]
        crossing = [(a, n, 0, tokens) for a, n in far]
        a, n = far[-1]
        crossing[-1:] = [(a, n, 0, tokens // 2), (a, n, tokens // 2, tokens // 2)]
        nx = len(crossing)
        pieces = [1] * (total - 2) + [depth] * 2
        first_z, relays = FIRST_Z, RELAYS
        factor = 1.0 / float(tokens * reps) ** 0.5
        dma = lambda n: pltpu.SemaphoreType.DMA((n,))
        vm = pltpu.VMEM
        results = pl.pallas_call(
            functools.partial(kernel, depth, near, far, crossing, marks, first_z, pieces, relays, ORDER, factor),
            out_shape=[
                pltpu.VMEM((tokens, hid), BF16),
                pltpu.VMEM((block, width), F32),
            ],
            in_specs=[pl.BlockSpec(memory_space=pl.ANY)] * 3,
            out_specs=[pl.BlockSpec(memory_space=pltpu.VMEM)] * 2,
            scratch_shapes=[
                vm((tokens, hid), BF16),
                vm((2 * depth, tokens, block), BF16),
                vm((2 * depth * block, 2 * tokens), BF16),
                vm(down_weight.shape, BF16),
                vm((2, 2 * tokens, half), BF16),
                vm((tokens, hid), F32),
                vm((depth, block, width), BF16),
                vm((depth, block, width), BF16),
                vm((depth, block, width), F32),
                vm((depth, block, width), BF16),
                vm((depth, block, width), BF16),
                vm((block, near[0][1]), F32),
                vm((block, near[0][1]), BF16),
                vm((depth, block, far[-1][1]), F32),
                pltpu.SemaphoreType.REGULAR, dma(3), dma(8), dma(2), dma(nn), dma(nx), dma(nx),
                dma(sum(pieces)), dma(1 + total), dma(2),
            ],
            compiler_params=pltpu.CompilerParams(
                collective_id=0, has_side_effects=True, vmem_limit_bytes=56 * 1024 * 1024
            ),
            cost_estimate=pl.CostEstimate(
                flops=8 * tokens * hid * width // 2, bytes_accessed=40 * 1024 * 1024, transcendentals=0),
        )(pre_act, down_weight, cotangent)
        return pl.pallas_call(
            store,
            out_shape=[
                jax.ShapeDtypeStruct((tokens, hid), BF16),
                jax.ShapeDtypeStruct((block, width), F32),
            ],
            in_specs=[pl.BlockSpec(memory_space=pl.ANY)] * 2,
            out_specs=[pl.BlockSpec(memory_space=pl.ANY)] * 2,
            scratch_shapes=[dma(PARTS + 1)],
            compiler_params=pltpu.CompilerParams(vmem_limit_bytes=1024 * 1024),
            cost_estimate=pl.CostEstimate(flops=1, bytes_accessed=10 * 1024 * 1024, transcendentals=0),
        )(*results)

    return jax.shard_map(
        on_device,
        mesh=mesh,
        in_specs=(P("rep", ("fs", "tp")), P(("fs", "tp"), None), P("rep", ("fs", "tp"))),
        out_specs=(P("rep", ("fs", "tp")), P(("fs", "tp", "rep"), None)),
        check_vma=False,
    )
```

```python
import contextlib
import functools

import jax
import jax.numpy as jnp
from jax import lax
from jax.experimental import pallas as pl
from jax.experimental.pallas import tpu as pltpu
from jax.sharding import PartitionSpec as P

MESH = pl.DeviceIdType.MESH
CORES, ROWS = 2, 2
F32, BF16 = jnp.float32, jnp.bfloat16


NEAR, FAR = (4, 4, 4, 4), (4, 4, 2, 2, 2, 2)
CUTS = (2, 4)
FIRST_Z, RELAYS = 0, range(8)
ORDER = (
    "n0 A0 n1 A1",
    "o4 i4 B0 n2",
    "A2 n3 A3 B1",
    "g3 g0 x0 B2",
    "s1 f0 A4 B3",
    "t0 B4 g1 g2",
    "s2 t1 x1 f1",
    "A5 B5 v0 s3",
    "h0 h1 t2 h2",
    "h3 x2 s4 f2",
    "A6 B6 t3 x3",
    "s5 f3 A7 B7",
    "k0 t4 s6 k1",
    "k2 x4 t5 k3",
    "f4 A8 B8 x5",
    "s7 t6 s8.0 x6",
    "f5 s8.1 P9 f6",
    "A9 t7 s8.2 s8.3",
    "B9 e0 e1 s9.0",
    "s9.1 s9.2 s9.3 e2",
    "e3 L0 l8 l9",
)


def scope(name):
    return contextlib.nullcontext()


def chunks_of(width, sizes):
    out, at = [], 0
    for s in sizes:
        out.append((at, s))
        at += s
    assert at == width
    return out


def plain(pre_act, down_weight, cotangent):
    whole = lax.all_gather(cotangent, ("fs", "tp"), axis=1, tiled=True)
    grad_hidden = lax.dot_general(
        whole, down_weight, (((1,), (1,)), ((), ())), preferred_element_type=F32
    )
    positive = jnp.maximum(pre_act.astype(F32), 0.0)
    grad_pre = (grad_hidden * 2.0 * positive).astype(BF16)
    hidden = (positive * positive).astype(BF16)
    factor = 1.0 / jnp.sqrt(jnp.float32(pre_act.shape[0] * lax.axis_size("rep")))
    term = lax.dot_general(
        hidden, whole, (((0,), (0,)), ((), ())), preferred_element_type=F32
    )
    summed = lax.psum_scatter(term, "rep", scatter_dimension=0, tiled=True)
    return (grad_pre, summed * factor)


def kernel(
    depth, near, far, crossing, marks, first_z, pieces, relays, order, factor,
    pre_hbm, w_hbm, cot_hbm, gp, gw,
    pre, pre_in, turned, w, cot, grad,
    y_out, y_in, own, z_out, z_in, b_sum, b_in, part,
    s_above, s_local, s_sent, s_pre_r, s_near_r, s_x_r, s_fwd_r, s_y_r, s_z_r, s_b_r,
):
    rep, fs, tp = lax.axis_index("rep"), lax.axis_index("fs"), lax.axis_index("tp")
    c, y, z = rep % CORES, (rep // CORES) % ROWS, rep // (CORES * ROWS)
    tokens, half = cot_hbm.shape
    hid = w_hbm.shape[0]
    block = own.shape[1]
    blocks = 2 * depth

    def at(z_, y_, c_, f_):
        return ((z_ * ROWS + y_) * CORES + c_, f_, tp)

    partner, across, beside = at(z, y, 1 - c, fs), at(z, y, c, 1 - fs), at(z, 1 - y, c, fs)

    def remote(src, dst, s, r, to):
        return pltpu.make_async_remote_copy(
            src_ref=src, dst_ref=dst, send_sem=s, recv_sem=r, device_id=to, device_id_type=MESH
        )

    def columns(i, c_):
        y_ = (1 - y) if i < depth else y
        k = (i % depth) * ROWS + y_
        return pl.ds(pl.multiple_of((k * CORES + c_) * block, block), block)

    def local(i, src, dst):
        return pltpu.make_async_copy(src, dst, s_local.at[i])

    loads = [local(0, cot_hbm, cot.at[0, pl.ds(0, tokens)]), local(1, pre_hbm, pre), local(2, w_hbm, w)]
    for l in loads:
        l.start()

    barrier = pltpu.get_barrier_semaphore()
    for p in (partner, across, beside):
        pl.semaphore_signal(barrier, inc=1, device_id=p, device_id_type=MESH)
    for d in range(1, depth):

        @pl.when(z + d < depth)
        def _(d=d):
            pl.semaphore_signal(barrier, inc=1, device_id=at(z + d, y, c, fs), device_id_type=MESH)

    with scope("bar"):
        pl.semaphore_wait(barrier, 3 + z)
    for d in range(1, depth):

        @pl.when(z >= d)
        def _(d=d):
            pl.semaphore_signal(s_above, inc=1, device_id=at(z - d, y, c, fs), device_id_type=MESH)

    x_copies = []
    for q, (a, n, r, rn) in enumerate(crossing):
        x_copies.append(remote(
            cot.at[0, pl.ds(r, rn), pl.ds(a, n)], cot.at[1, pl.ds(r, rn), pl.ds(a, n)],
            s_sent.at[2], s_x_r.at[q], across))
    pre_copies = []
    for i in range(blocks):
        pre_copies.append(remote(
            pre.at[:, columns(i, 1 - c)], pre_in.at[i], s_sent.at[0], s_pre_r.at[i // depth], partner))
    near_copies = []
    for q, (a, n) in enumerate(near):
        near_copies.append(remote(
            cot.at[0, pl.ds(0, tokens), pl.ds(a, n)], cot.at[0, pl.ds(tokens, tokens), pl.ds(a, n)],
            s_sent.at[1], s_near_r.at[q], partner))
    with scope("ld"):
        loads[0].wait()
    for xc in x_copies:
        xc.start()
    loads[1].wait()
    for group in (pre_copies[:depth], near_copies[:2], pre_copies[depth:], near_copies[2:]):
        for copy in group:
            copy.start()
    def turn(v):
        p = jnp.maximum(v.astype(F32), 0.0)
        return (p * p).T.astype(BF16)

    strip = 256

    def turn_own(first):
        for i in range(first, first + depth):
            cols = columns(i, c)

            @pl.loop(0, tokens // strip, unroll=2)
            def _(t):
                rows = pl.ds(pl.multiple_of(t * strip, strip), strip)
                turned[pl.ds(i * block, block), rows] = turn(pre[rows, cols])

    def turn_in(first):
        both = pre_in.at[pl.ds(first, depth)]
        remote(both, both, s_sent.at[0], s_pre_r.at[first // depth], partner).wait_recv()

        @pl.loop(first, first + depth)
        def _(i):
            @pl.loop(0, tokens // strip, unroll=2)
            def _(t):
                rows = pl.ds(pl.multiple_of(t * strip, strip), strip)
                to = pl.ds(pl.multiple_of(tokens + t * strip, strip), strip)
                turned[pl.ds(pl.multiple_of(i * block, block), block), to] = turn(pre_in[i, rows, :])

    tall = 2 * block

    chunks = [(0, a, n) for a, n in near] + [(1, a, n) for a, n in far]

    final = len(chunks) - 1

    def span(h, a, n):
        return pl.ds(h * half + a, n)

    def turn_of(p):
        return jnp.where(c == 0, p, p + 1 - 2 * (p % 2))

    def y_copy(j, p=0):
        h, a, n = chunks[j]
        s = span(h, a, n)
        if j == first_z:
            return remote(y_out.at[z, :, s], b_in, s_sent.at[5], s_y_r.at[sum(pieces[:j])], beside)
        rows = pl.ds(turn_of(p), 1) if pieces[j] > 1 else pl.ds(0, depth)
        return remote(
            y_out.at[rows, :, s], y_in.at[rows, :, s], s_sent.at[4], s_y_r.at[sum(pieces[:j]) + p], beside)

    slots, far_end = depth, depth - 1
    inner = (z > 0) & (z < far_end)

    def relayed(j):
        return j in relays

    def z_block(j, kind):
        if kind == "up":
            ends = (z == far_end) if relayed(j) else False
            return jnp.where(ends, 0, (z + 1) % depth), jnp.where(ends, 3, 0), jnp.where(ends, far_end - 1, (z + 1) % depth)
        if kind == "down":
            ends = (z == 0) if relayed(j) else False
            return jnp.where(ends, far_end, (z + far_end) % depth), jnp.where(ends, 3, 2), jnp.where(ends, 1, (z + far_end) % depth)
        return (z + 2) % depth, 1, (z + 2) % depth

    def z_copy(j, kind, of_beside=False):
        h, a, n = chunks[j]
        s = span(h, a, n)
        block_, slot, to = z_block(j, kind)
        relay = jnp.where(slot == 3, 1, 0)
        if of_beside:
            return remote(
                y_out.at[block_, :, s], y_in.at[slot, :, s], s_sent.at[7], s_b_r.at[relay], at(to, y, c, fs))
        return remote(
            z_out.at[block_, :, s], z_in.at[slot, :, s],
            s_sent.at[6], s_z_r.at[relay * (1 + j) if relayed(j) else 1 + j], at(to, y, c, fs))

    def arrived(ref, sem):
        remote(ref, ref, s_sent.at[6], sem, beside).wait_recv()

    def all_arrived(ref, cols, sem):
        pl.when(inner)(lambda: arrived(ref.at[pl.ds(0, 3), :, cols], sem))
        pl.when(jnp.logical_not(inner))(lambda: arrived(ref.at[pl.ds(0, 2), :, cols], sem))

    def z_send(j, of_beside=False):
        z_copy(j, "up", of_beside).start()
        z_copy(j, "down", of_beside).start()
        if relayed(j):

            @pl.when(jnp.logical_not(inner))
            def _():
                z_copy(j, "two", of_beside).start()
        else:
            z_copy(j, "two", of_beside).start()

    def fwd_copy(q):
        a, n, r, rn = crossing[q]
        return remote(
            cot.at[1, pl.ds(r, rn), pl.ds(a, n)], cot.at[1, pl.ds(tokens + r, rn), pl.ds(a, n)],
            s_sent.at[3], s_fwd_r.at[q], partner)

    def dot(j, m, which=None):
        h, a, n = chunks[j]
        rows = pl.ds(pl.multiple_of(m * tall, tall), tall)
        if which is None:
            return lax.dot_general(
                turned[rows, :], cot[h, :, pl.ds(a, n)], (((1,), (0,)), ((), ())),
                preferred_element_type=F32).reshape(2, block, n)
        r, rn = crossing[which][2:]

        def over(first):
            ts = pl.ds(first + r, rn)
            return lax.dot_general(
                turned[rows, ts], cot[h, ts, pl.ds(a, n)], (((1,), (0,)), ((), ())),
                preferred_element_type=F32)

        return (over(0) + over(tokens)).reshape(2, block, n)

    def product_start(j):
        h, a, n = chunks[j]
        s = span(h, a, n)
        for m in range(depth // 2):
            part[pl.ds(m * 2, 2)] = dot(j, m, -2)
            own[pl.ds(m * 2, 2), :, s] = dot(j, m + depth // 2, -2)

    def product_beside(j):
        h, a, n = chunks[j]
        s = span(h, a, n)
        if pieces[j] > 1:
            for m in range(depth // 2):
                v = part[pl.ds(m * 2, 2)] + dot(j, m, -1) if j == final else dot(j, m)
                y_out[pl.ds(m * 2, 2), :, s] = v.astype(BF16)
                y_copy(j, 2 * m).start()
                y_copy(j, 2 * m + 1).start()
            return

        @pl.loop(0, depth // 2, unroll=True)
        def _(m):
            y_out[pl.ds(m * 2, 2), :, s] = dot(j, m).astype(BF16)

        if j == first_z:
            b_sum[...] = y_out[z, :, s].astype(F32)
            z_send(j, True)
        else:
            y_copy(j).start()

    def product_own(j):
        h, a, n = chunks[j]
        s = span(h, a, n)
        if j == final:
            for m in range(depth // 2):
                own[pl.ds(m * 2, 2), :, s] += dot(j, m + depth // 2, -1)
            return

        @pl.loop(0, depth // 2, unroll=True)
        def _(m):
            v = dot(j, m + depth // 2)
            own[pl.ds(m * 2, 2), :, s] = v
            if j == first_z:
                z_out[pl.ds(m * 2, 2), :, s] = v.astype(BF16)

        if j == first_z:
            z_send(j)

    def second(j, p=0):
        h, a, n = chunks[j]
        s = span(h, a, n)
        with scope(f"wy{j}"):
            y_copy(j, p).wait_recv()

        def add(k):
            v = own[k, :, s] + y_in[k, :, s].astype(F32)
            own[k, :, s] = v
            z_out[k, :, s] = v.astype(BF16)

        if pieces[j] == 1:
            pl.loop(0, depth)(add)
            z_send(j)
            return
        k = turn_of(p)
        add(k)
        for kind in ("up", "down", "two"):

            @pl.when(z_block(j, kind)[0] == k)
            def _(kind=kind):
                z_copy(j, kind).start()

    def third(j):
        h, a, n = chunks[j]
        s = span(h, a, n)

        @pl.when(inner)
        def _():
            to = (z + 2) % depth
            with scope(f"wr{j}"):
                arrived(z_in.at[3, :, s], s_z_r.at[1 + j])
            z_out[to, :, s] = (own[to, :, s] + z_in[3, :, s].astype(F32)).astype(BF16)
            z_copy(j, "two").start()
            if j == first_z:
                arrived(y_in.at[3, :, s], s_b_r.at[1])
                y_out[to, :, s] = (y_out[to, :, s].astype(F32) + y_in[3, :, s].astype(F32)).astype(BF16)
                z_copy(j, "two", True).start()

    def arrivals(j, add):
        for slot, there in ((0, z > 0), (2, z < far_end), (1, None)) if relayed(j) else ((0, None), (2, None), (1, None)):
            if there is None:
                add(slot)
            else:
                pl.when(there)(functools.partial(add, slot))

    def across_z(j):
        h, a, n = chunks[j]
        s = span(h, a, n)
        with scope("wb"):
            all_arrived(y_in, s, s_b_r.at[0])

        def add(slot):
            b_sum[...] += y_in[slot, :, s].astype(F32)

        arrivals(j, add)
        y_out[z, :, s] = b_sum[...].astype(BF16)
        y_copy(j).start()

    def total_of(j):
        h, a, n = chunks[j]
        s = span(h, a, n)

        def add(slot):
            own[z, :, s] = own[z, :, s] + z_in[slot, :, s].astype(F32)

        arrivals(j, add)
        place = pl.multiple_of((fs if h == 0 else 1 - fs) * half + a, 128)
        v = own[z, :, s]
        if j == first_z:
            v = v + b_in[...].astype(F32)
        gw[:, pl.ds(place, n)] = v * factor

    def last(j):
        h, a, n = chunks[j]
        with scope(f"wz{j}"):
            arrived(z_in.at[pl.ds(0, 3), :, span(h, a, n)], s_z_r.at[1 + j])
        total_of(j)

    def last_relayed(_):
        h, a, n = chunks[len(relays) - 1]
        with scope("wL"):
            all_arrived(z_in, pl.ds(0, h * half + a + n), s_z_r.at[0])
        with scope("wLy"):
            if first_z is not None:
                y_copy(first_z).wait_recv()
        for j in relays:
            total_of(j)

    tm, tn = 256, 512

    def grad_tile(h, a, n, m, k):
        rows = pl.ds(pl.multiple_of(m * tm, tm), tm)
        outs = pl.ds(pl.multiple_of(k * tn, tn), tn)
        place = pl.multiple_of((fs if h == 0 else 1 - fs) * half + a, 128)
        return rows, outs, lax.dot_general(
            cot[h, rows, pl.ds(a, n)], w[outs, pl.ds(place, n)], (((1,), (1,)), ((), ())),
            preferred_element_type=F32)

    weights = [loads[2]]

    def grad_first(m):
        if weights:
            weights.pop().wait()

        @pl.loop(0, hid // tn, unroll=True)
        def _(k):
            rows, outs, v = grad_tile(0, 0, half, m, k)
            grad[rows, outs] = v

    def grad_next(m, part):
        @pl.loop(0, hid // tn, unroll=True)
        def _(k):
            rows, outs, v = grad_tile(1, marks[part], marks[part + 1] - marks[part], m, k)
            grad[rows, outs] += v

    def grad_rest(m):
        @pl.loop(0, hid // tn, unroll=True)
        def _(k):
            rows, outs, v = grad_tile(1, marks[-2], marks[-1] - marks[-2], m, k)
            p = jnp.maximum(pre[rows, outs].astype(F32), 0.0)
            gp[rows, outs] = ((grad[rows, outs] + v) * 2.0 * p).astype(BF16)

    def near_in(q):
        near_copies[q].wait_recv()

    def far_in(q):
        x_copies[q].wait_recv()
        fwd_copy(q).start()

    def far_both(q):
        fwd_copy(q).wait_recv()

    nn, nf = len(near), len(far)
    total = nn + nf
    steps = {
        "A": product_beside, "B": product_own, "P": product_start,
        "s": second, "t": third, "v": across_z, "l": last, "L": last_relayed, "n": near_in, "x": far_in, "f": far_both,
        "g": grad_first, "h": lambda m: grad_next(m, 0), "k": lambda m: grad_next(m, 1), "e": grad_rest,
        "o": turn_own, "i": turn_in,
    }
    with scope("o0"):
        turn_own(0)
    with scope("i0"):
        turn_in(0)
    with scope("above"):
        pl.when(z < depth - 1)(lambda: pl.semaphore_wait(s_above, depth - 1 - z))
    for step in " ".join(order).split():
        with scope(step):
            steps[step[0]](*(int(v) for v in step[1:].split(".")))

    with scope("drain"):
        skip = 0 if first_z is None else near[0][1]
        whole = cot.at[0, pl.ds(0, tokens)]
        first = pl.ds(0, skip)
        sent = [
            pre.at[:, pl.ds(0, blocks * block)], whole, whole, whole,
            y_out.at[:, :, pl.ds(skip, 2 * half - skip)], y_out.at[0, :, first],
            z_out.at[pl.ds(0, 3)], y_out.at[pl.ds(0, 3), :, first],
        ]
        for i, ref in enumerate(sent):
            if skip or i not in (5, 7):
                remote(ref, ref, s_sent.at[i], s_b_r.at[0], partner).wait_send()


PARTS = 4


def store(gp_in, gw_in, gp_out, gw_out, sems):
    rows = gp_in.shape[0] // PARTS
    copies = [pltpu.make_async_copy(gw_in, gw_out, sems.at[PARTS])]
    for i in range(PARTS):
        r = pl.ds(i * rows, rows)
        copies.append(pltpu.make_async_copy(gp_in.at[r], gp_out.at[r], sems.at[i]))
    for copy in copies:
        copy.start()
    for copy in copies:
        copy.wait()


def solution(mesh):
    reps, fs, tp = mesh.shape["rep"], mesh.shape["fs"], mesh.shape["tp"]
    depth = reps // (CORES * ROWS)

    def on_device(pre_act, down_weight, cotangent):
        tokens, hid = pre_act.shape
        half = cotangent.shape[1]
        width = down_weight.shape[1]
        block = hid // reps
        if not (fs == 2 and tp == 1 and depth * CORES * ROWS == reps and depth == 4
                and block % 128 == 0 and half % 1024 == 0 and hid % 512 == 0 and tokens == 1024):
            return plain(pre_act, down_weight, cotangent)
        step = half // 4
        near = chunks_of(half, [step // 4 * v for v in NEAR])
        far = chunks_of(half, [step // 4 * v for v in FAR])
        nn, nf = len(near), len(far)
        total = nn + nf
        marks = [0] + [far[i][0] for i in CUTS] + [half]
        crossing = [(a, n, 0, tokens) for a, n in far]
        a, n = far[-1]
        crossing[-1:] = [(a, n, 0, tokens // 2), (a, n, tokens // 2, tokens // 2)]
        nx = len(crossing)
        pieces = [1] * (total - 2) + [depth] * 2
        first_z, relays = FIRST_Z, RELAYS
        factor = 1.0 / float(tokens * reps) ** 0.5
        dma = lambda n: pltpu.SemaphoreType.DMA((n,))
        vm = pltpu.VMEM
        results = pl.pallas_call(
            functools.partial(kernel, depth, near, far, crossing, marks, first_z, pieces, relays, ORDER, factor),
            out_shape=[
                pltpu.VMEM((tokens, hid), BF16),
                pltpu.VMEM((block, width), F32),
            ],
            in_specs=[pl.BlockSpec(memory_space=pl.ANY)] * 3,
            out_specs=[pl.BlockSpec(memory_space=pltpu.VMEM)] * 2,
            scratch_shapes=[
                vm((tokens, hid), BF16),
                vm((2 * depth, tokens, block), BF16),
                vm((2 * depth * block, 2 * tokens), BF16),
                vm(down_weight.shape, BF16),
                vm((2, 2 * tokens, half), BF16),
                vm((tokens, hid), F32),
                vm((depth, block, width), BF16),
                vm((depth, block, width), BF16),
                vm((depth, block, width), F32),
                vm((depth, block, width), BF16),
                vm((depth, block, width), BF16),
                vm((block, near[0][1]), F32),
                vm((block, near[0][1]), BF16),
                vm((depth, block, far[-1][1]), F32),
                pltpu.SemaphoreType.REGULAR, dma(3), dma(8), dma(2), dma(nn), dma(nx), dma(nx),
                dma(sum(pieces)), dma(1 + total), dma(2),
            ],
            compiler_params=pltpu.CompilerParams(
                collective_id=0, has_side_effects=True, vmem_limit_bytes=56 * 1024 * 1024
            ),
            cost_estimate=pl.CostEstimate(
                flops=8 * tokens * hid * width // 2, bytes_accessed=40 * 1024 * 1024, transcendentals=0),
        )(pre_act, down_weight, cotangent)
        return pl.pallas_call(
            store,
            out_shape=[
                jax.ShapeDtypeStruct((tokens, hid), BF16),
                jax.ShapeDtypeStruct((block, width), F32),
            ],
            in_specs=[pl.BlockSpec(memory_space=pl.ANY)] * 2,
            out_specs=[pl.BlockSpec(memory_space=pl.ANY)] * 2,
            scratch_shapes=[dma(PARTS + 1)],
            compiler_params=pltpu.CompilerParams(vmem_limit_bytes=1024 * 1024),
            cost_estimate=pl.CostEstimate(flops=1, bytes_accessed=10 * 1024 * 1024, transcendentals=0),
        )(*results)

    return jax.shard_map(
        on_device,
        mesh=mesh,
        in_specs=(P("rep", ("fs", "tp")), P(("fs", "tp"), None), P("rep", ("fs", "tp"))),
        out_specs=(P("rep", ("fs", "tp")), P(("fs", "tp", "rep"), None)),
        check_vma=False,
    )
```

```python
import contextlib
import functools

import jax
import jax.numpy as jnp
from jax import lax
from jax.experimental import pallas as pl
from jax.experimental.pallas import tpu as pltpu
from jax.sharding import PartitionSpec as P

MESH = pl.DeviceIdType.MESH
CORES, ROWS = 2, 2
F32, BF16 = jnp.float32, jnp.bfloat16


NEAR, FAR = (4, 4, 4, 4), (4, 4, 2, 2, 2, 2)
CUTS = (2, 4)
FIRST_Z, RELAYS = 0, range(7)
ORDER = (
    "n0 A0 n1 A1",
    "o4 i4 B0 n2",
    "A2 n3 A3 B1",
    "g3 g0 x0 B2",
    "s1 f0 A4 B3",
    "t0 B4 g1 g2",
    "s2 t1 x1 f1",
    "A5 B5 v0 s3",
    "h0 h1 t2 h2",
    "h3 x2 s4 f2",
    "A6 B6 t3 x3",
    "s5 f3 A7 B7",
    "k0 t4 s6 k1",
    "k2 x4 t5 k3",
    "f4 A8 B8 x5",
    "s7 t6 s8.0 x6",
    "f5 s8.1 P9 f6",
    "A9 s8.2 s8.3 B9",
    "e0 e1 s9.0 s9.1",
    "s9.2 s9.3 e2 e3",
    "L0 l7 l8 l9",
)


def scope(name):
    return contextlib.nullcontext()


def chunks_of(width, sizes):
    out, at = [], 0
    for s in sizes:
        out.append((at, s))
        at += s
    assert at == width
    return out


def plain(pre_act, down_weight, cotangent):
    whole = lax.all_gather(cotangent, ("fs", "tp"), axis=1, tiled=True)
    grad_hidden = lax.dot_general(
        whole, down_weight, (((1,), (1,)), ((), ())), preferred_element_type=F32
    )
    positive = jnp.maximum(pre_act.astype(F32), 0.0)
    grad_pre = (grad_hidden * 2.0 * positive).astype(BF16)
    hidden = (positive * positive).astype(BF16)
    factor = 1.0 / jnp.sqrt(jnp.float32(pre_act.shape[0] * lax.axis_size("rep")))
    term = lax.dot_general(
        hidden, whole, (((0,), (0,)), ((), ())), preferred_element_type=F32
    )
    summed = lax.psum_scatter(term, "rep", scatter_dimension=0, tiled=True)
    return (grad_pre, summed * factor)


def kernel(
    depth, near, far, crossing, marks, first_z, pieces, relays, order, factor,
    pre_hbm, w_hbm, cot_hbm, gp, gw,
    pre, pre_in, turned, w, cot, grad,
    y_out, y_in, own, z_out, z_in, b_sum, b_in, part,
    s_above, s_local, s_sent, s_pre_r, s_near_r, s_x_r, s_fwd_r, s_y_r, s_z_r, s_b_r,
):
    rep, fs, tp = lax.axis_index("rep"), lax.axis_index("fs"), lax.axis_index("tp")
    c, y, z = rep % CORES, (rep // CORES) % ROWS, rep // (CORES * ROWS)
    tokens, half = cot_hbm.shape
    hid = w_hbm.shape[0]
    block = own.shape[1]
    blocks = 2 * depth

    def at(z_, y_, c_, f_):
        return ((z_ * ROWS + y_) * CORES + c_, f_, tp)

    partner, across, beside = at(z, y, 1 - c, fs), at(z, y, c, 1 - fs), at(z, 1 - y, c, fs)

    def remote(src, dst, s, r, to):
        return pltpu.make_async_remote_copy(
            src_ref=src, dst_ref=dst, send_sem=s, recv_sem=r, device_id=to, device_id_type=MESH
        )

    def columns(i, c_):
        y_ = (1 - y) if i < depth else y
        k = (i % depth) * ROWS + y_
        return pl.ds(pl.multiple_of((k * CORES + c_) * block, block), block)

    def local(i, src, dst):
        return pltpu.make_async_copy(src, dst, s_local.at[i])

    loads = [local(0, cot_hbm, cot.at[0, pl.ds(0, tokens)]), local(1, pre_hbm, pre), local(2, w_hbm, w)]
    for l in loads:
        l.start()

    barrier = pltpu.get_barrier_semaphore()
    for p in (partner, across, beside):
        pl.semaphore_signal(barrier, inc=1, device_id=p, device_id_type=MESH)
    for d in range(1, depth):

        @pl.when(z + d < depth)
        def _(d=d):
            pl.semaphore_signal(barrier, inc=1, device_id=at(z + d, y, c, fs), device_id_type=MESH)

    with scope("bar"):
        pl.semaphore_wait(barrier, 3 + z)
    for d in range(1, depth):

        @pl.when(z >= d)
        def _(d=d):
            pl.semaphore_signal(s_above, inc=1, device_id=at(z - d, y, c, fs), device_id_type=MESH)

    x_copies = []
    for q, (a, n, r, rn) in enumerate(crossing):
        x_copies.append(remote(
            cot.at[0, pl.ds(r, rn), pl.ds(a, n)], cot.at[1, pl.ds(r, rn), pl.ds(a, n)],
            s_sent.at[2], s_x_r.at[q], across))
    pre_copies = []
    for i in range(blocks):
        pre_copies.append(remote(
            pre.at[:, columns(i, 1 - c)], pre_in.at[i], s_sent.at[0], s_pre_r.at[i // depth], partner))
    near_copies = []
    for q, (a, n) in enumerate(near):
        near_copies.append(remote(
            cot.at[0, pl.ds(0, tokens), pl.ds(a, n)], cot.at[0, pl.ds(tokens, tokens), pl.ds(a, n)],
            s_sent.at[1], s_near_r.at[q], partner))
    with scope("ld"):
        loads[0].wait()
    for xc in x_copies:
        xc.start()
    loads[1].wait()
    for group in (pre_copies[:depth], near_copies[:2], pre_copies[depth:], near_copies[2:]):
        for copy in group:
            copy.start()
    def turn(v):
        p = jnp.maximum(v.astype(F32), 0.0)
        return (p * p).T.astype(BF16)

    strip = 256

    def turn_own(first):
        for i in range(first, first + depth):
            cols = columns(i, c)

            @pl.loop(0, tokens // strip, unroll=2)
            def _(t):
                rows = pl.ds(pl.multiple_of(t * strip, strip), strip)
                turned[pl.ds(i * block, block), rows] = turn(pre[rows, cols])

    def turn_in(first):
        both = pre_in.at[pl.ds(first, depth)]
        remote(both, both, s_sent.at[0], s_pre_r.at[first // depth], partner).wait_recv()

        @pl.loop(first, first + depth)
        def _(i):
            @pl.loop(0, tokens // strip, unroll=2)
            def _(t):
                rows = pl.ds(pl.multiple_of(t * strip, strip), strip)
                to = pl.ds(pl.multiple_of(tokens + t * strip, strip), strip)
                turned[pl.ds(pl.multiple_of(i * block, block), block), to] = turn(pre_in[i, rows, :])

    tall = 2 * block

    chunks = [(0, a, n) for a, n in near] + [(1, a, n) for a, n in far]

    final = len(chunks) - 1

    def span(h, a, n):
        return pl.ds(h * half + a, n)

    def turn_of(p):
        return jnp.where(c == 0, p, p + 1 - 2 * (p % 2))

    def y_copy(j, p=0):
        h, a, n = chunks[j]
        s = span(h, a, n)
        if j == first_z:
            return remote(y_out.at[z, :, s], b_in, s_sent.at[5], s_y_r.at[sum(pieces[:j])], beside)
        rows = pl.ds(turn_of(p), 1) if pieces[j] > 1 else pl.ds(0, depth)
        return remote(
            y_out.at[rows, :, s], y_in.at[rows, :, s], s_sent.at[4], s_y_r.at[sum(pieces[:j]) + p], beside)

    slots, far_end = depth, depth - 1
    inner = (z > 0) & (z < far_end)

    def relayed(j):
        return j in relays

    def z_block(j, kind):
        if kind == "up":
            ends = (z == far_end) if relayed(j) else False
            return jnp.where(ends, 0, (z + 1) % depth), jnp.where(ends, 3, 0), jnp.where(ends, far_end - 1, (z + 1) % depth)
        if kind == "down":
            ends = (z == 0) if relayed(j) else False
            return jnp.where(ends, far_end, (z + far_end) % depth), jnp.where(ends, 3, 2), jnp.where(ends, 1, (z + far_end) % depth)
        return (z + 2) % depth, 1, (z + 2) % depth

    def z_copy(j, kind, of_beside=False):
        h, a, n = chunks[j]
        s = span(h, a, n)
        block_, slot, to = z_block(j, kind)
        relay = jnp.where(slot == 3, 1, 0)
        if of_beside:
            return remote(
                y_out.at[block_, :, s], y_in.at[slot, :, s], s_sent.at[7], s_b_r.at[relay], at(to, y, c, fs))
        return remote(
            z_out.at[block_, :, s], z_in.at[slot, :, s],
            s_sent.at[6], s_z_r.at[relay * (1 + j) if relayed(j) else 1 + j], at(to, y, c, fs))

    def arrived(ref, sem):
        remote(ref, ref, s_sent.at[6], sem, beside).wait_recv()

    def all_arrived(ref, cols, sem):
        pl.when(inner)(lambda: arrived(ref.at[pl.ds(0, 3), :, cols], sem))
        pl.when(jnp.logical_not(inner))(lambda: arrived(ref.at[pl.ds(0, 2), :, cols], sem))

    def z_send(j, of_beside=False):
        z_copy(j, "up", of_beside).start()
        z_copy(j, "down", of_beside).start()
        if relayed(j):

            @pl.when(jnp.logical_not(inner))
            def _():
                z_copy(j, "two", of_beside).start()
        else:
            z_copy(j, "two", of_beside).start()

    def fwd_copy(q):
        a, n, r, rn = crossing[q]
        return remote(
            cot.at[1, pl.ds(r, rn), pl.ds(a, n)], cot.at[1, pl.ds(tokens + r, rn), pl.ds(a, n)],
            s_sent.at[3], s_fwd_r.at[q], partner)

    def dot(j, m, which=None):
        h, a, n = chunks[j]
        rows = pl.ds(pl.multiple_of(m * tall, tall), tall)
        if which is None:
            return lax.dot_general(
                turned[rows, :], cot[h, :, pl.ds(a, n)], (((1,), (0,)), ((), ())),
                preferred_element_type=F32).reshape(2, block, n)
        r, rn = crossing[which][2:]

        def over(first):
            ts = pl.ds(first + r, rn)
            return lax.dot_general(
                turned[rows, ts], cot[h, ts, pl.ds(a, n)], (((1,), (0,)), ((), ())),
                preferred_element_type=F32)

        return (over(0) + over(tokens)).reshape(2, block, n)

    def product_start(j):
        h, a, n = chunks[j]
        s = span(h, a, n)
        for m in range(depth // 2):
            part[pl.ds(m * 2, 2)] = dot(j, m, -2)
            own[pl.ds(m * 2, 2), :, s] = dot(j, m + depth // 2, -2)

    def product_beside(j):
        h, a, n = chunks[j]
        s = span(h, a, n)
        if pieces[j] > 1:
            for m in range(depth // 2):
                v = part[pl.ds(m * 2, 2)] + dot(j, m, -1) if j == final else dot(j, m)
                y_out[pl.ds(m * 2, 2), :, s] = v.astype(BF16)
                y_copy(j, 2 * m).start()
                y_copy(j, 2 * m + 1).start()
            return

        @pl.loop(0, depth // 2, unroll=True)
        def _(m):
            y_out[pl.ds(m * 2, 2), :, s] = dot(j, m).astype(BF16)

        if j == first_z:
            b_sum[...] = y_out[z, :, s].astype(F32)
            z_send(j, True)
        else:
            y_copy(j).start()

    def product_own(j):
        h, a, n = chunks[j]
        s = span(h, a, n)
        if j == final:
            for m in range(depth // 2):
                own[pl.ds(m * 2, 2), :, s] += dot(j, m + depth // 2, -1)
            return

        @pl.loop(0, depth // 2, unroll=True)
        def _(m):
            v = dot(j, m + depth // 2)
            own[pl.ds(m * 2, 2), :, s] = v
            if j == first_z:
                z_out[pl.ds(m * 2, 2), :, s] = v.astype(BF16)

        if j == first_z:
            z_send(j)

    def second(j, p=0):
        h, a, n = chunks[j]
        s = span(h, a, n)
        with scope(f"wy{j}"):
            y_copy(j, p).wait_recv()

        def add(k):
            v = own[k, :, s] + y_in[k, :, s].astype(F32)
            own[k, :, s] = v
            z_out[k, :, s] = v.astype(BF16)

        if pieces[j] == 1:
            pl.loop(0, depth)(add)
            z_send(j)
            return
        k = turn_of(p)
        add(k)
        for kind in ("up", "down", "two"):

            @pl.when(z_block(j, kind)[0] == k)
            def _(kind=kind):
                z_copy(j, kind).start()

    def third(j):
        h, a, n = chunks[j]
        s = span(h, a, n)

        @pl.when(inner)
        def _():
            to = (z + 2) % depth
            with scope(f"wr{j}"):
                arrived(z_in.at[3, :, s], s_z_r.at[1 + j])
            z_out[to, :, s] = (own[to, :, s] + z_in[3, :, s].astype(F32)).astype(BF16)
            z_copy(j, "two").start()
            if j == first_z:
                arrived(y_in.at[3, :, s], s_b_r.at[1])
                y_out[to, :, s] = (y_out[to, :, s].astype(F32) + y_in[3, :, s].astype(F32)).astype(BF16)
                z_copy(j, "two", True).start()

    def arrivals(j, add):
        for slot, there in ((0, z > 0), (2, z < far_end), (1, None)) if relayed(j) else ((0, None), (2, None), (1, None)):
            if there is None:
                add(slot)
            else:
                pl.when(there)(functools.partial(add, slot))

    def across_z(j):
        h, a, n = chunks[j]
        s = span(h, a, n)
        with scope("wb"):
            all_arrived(y_in, s, s_b_r.at[0])

        def add(slot):
            b_sum[...] += y_in[slot, :, s].astype(F32)

        arrivals(j, add)
        y_out[z, :, s] = b_sum[...].astype(BF16)
        y_copy(j).start()

    def total_of(j):
        h, a, n = chunks[j]
        s = span(h, a, n)

        def add(slot):
            own[z, :, s] = own[z, :, s] + z_in[slot, :, s].astype(F32)

        arrivals(j, add)
        place = pl.multiple_of((fs if h == 0 else 1 - fs) * half + a, 128)
        v = own[z, :, s]
        if j == first_z:
            v = v + b_in[...].astype(F32)
        gw[:, pl.ds(place, n)] = v * factor

    def last(j):
        h, a, n = chunks[j]
        with scope(f"wz{j}"):
            arrived(z_in.at[pl.ds(0, 3), :, span(h, a, n)], s_z_r.at[1 + j])
        total_of(j)

    def last_relayed(_):
        h, a, n = chunks[len(relays) - 1]
        with scope("wL"):
            all_arrived(z_in, pl.ds(0, h * half + a + n), s_z_r.at[0])
        with scope("wLy"):
            if first_z is not None:
                y_copy(first_z).wait_recv()
        for j in relays:
            total_of(j)

    tm, tn = 256, 512

    def grad_tile(h, a, n, m, k):
        rows = pl.ds(pl.multiple_of(m * tm, tm), tm)
        outs = pl.ds(pl.multiple_of(k * tn, tn), tn)
        place = pl.multiple_of((fs if h == 0 else 1 - fs) * half + a, 128)
        return rows, outs, lax.dot_general(
            cot[h, rows, pl.ds(a, n)], w[outs, pl.ds(place, n)], (((1,), (1,)), ((), ())),
            preferred_element_type=F32)

    weights = [loads[2]]

    def grad_first(m):
        if weights:
            weights.pop().wait()

        @pl.loop(0, hid // tn, unroll=True)
        def _(k):
            rows, outs, v = grad_tile(0, 0, half, m, k)
            grad[rows, outs] = v

    def grad_next(m, part):
        @pl.loop(0, hid // tn, unroll=True)
        def _(k):
            rows, outs, v = grad_tile(1, marks[part], marks[part + 1] - marks[part], m, k)
            grad[rows, outs] += v

    def grad_rest(m):
        @pl.loop(0, hid // tn, unroll=True)
        def _(k):
            rows, outs, v = grad_tile(1, marks[-2], marks[-1] - marks[-2], m, k)
            p = jnp.maximum(pre[rows, outs].astype(F32), 0.0)
            gp[rows, outs] = ((grad[rows, outs] + v) * 2.0 * p).astype(BF16)

    def near_in(q):
        near_copies[q].wait_recv()

    def far_in(q):
        x_copies[q].wait_recv()
        fwd_copy(q).start()

    def far_both(q):
        fwd_copy(q).wait_recv()

    nn, nf = len(near), len(far)
    total = nn + nf
    steps = {
        "A": product_beside, "B": product_own, "P": product_start,
        "s": second, "t": third, "v": across_z, "l": last, "L": last_relayed, "n": near_in, "x": far_in, "f": far_both,
        "g": grad_first, "h": lambda m: grad_next(m, 0), "k": lambda m: grad_next(m, 1), "e": grad_rest,
        "o": turn_own, "i": turn_in,
    }
    with scope("o0"):
        turn_own(0)
    with scope("i0"):
        turn_in(0)
    with scope("above"):
        pl.when(z < depth - 1)(lambda: pl.semaphore_wait(s_above, depth - 1 - z))
    for step in " ".join(order).split():
        with scope(step):
            steps[step[0]](*(int(v) for v in step[1:].split(".")))

    with scope("drain"):
        skip = 0 if first_z is None else near[0][1]
        whole = cot.at[0, pl.ds(0, tokens)]
        first = pl.ds(0, skip)
        sent = [
            pre.at[:, pl.ds(0, blocks * block)], whole, whole, whole,
            y_out.at[:, :, pl.ds(skip, 2 * half - skip)], y_out.at[0, :, first],
            z_out.at[pl.ds(0, 3)], y_out.at[pl.ds(0, 3), :, first],
        ]
        for i, ref in enumerate(sent):
            if skip or i not in (5, 7):
                remote(ref, ref, s_sent.at[i], s_b_r.at[0], partner).wait_send()


PARTS = 4


def store(gp_in, gw_in, gp_out, gw_out, sems):
    rows = gp_in.shape[0] // PARTS
    copies = [pltpu.make_async_copy(gw_in, gw_out, sems.at[PARTS])]
    for i in range(PARTS):
        r = pl.ds(i * rows, rows)
        copies.append(pltpu.make_async_copy(gp_in.at[r], gp_out.at[r], sems.at[i]))
    for copy in copies:
        copy.start()
    for copy in copies:
        copy.wait()


def solution(mesh):
    reps, fs, tp = mesh.shape["rep"], mesh.shape["fs"], mesh.shape["tp"]
    depth = reps // (CORES * ROWS)

    def on_device(pre_act, down_weight, cotangent):
        tokens, hid = pre_act.shape
        half = cotangent.shape[1]
        width = down_weight.shape[1]
        block = hid // reps
        if not (fs == 2 and tp == 1 and depth * CORES * ROWS == reps and depth == 4
                and block % 128 == 0 and half % 1024 == 0 and hid % 512 == 0 and tokens == 1024):
            return plain(pre_act, down_weight, cotangent)
        step = half // 4
        near = chunks_of(half, [step // 4 * v for v in NEAR])
        far = chunks_of(half, [step // 4 * v for v in FAR])
        nn, nf = len(near), len(far)
        total = nn + nf
        marks = [0] + [far[i][0] for i in CUTS] + [half]
        crossing = [(a, n, 0, tokens) for a, n in far]
        a, n = far[-1]
        crossing[-1:] = [(a, n, 0, tokens // 2), (a, n, tokens // 2, tokens // 2)]
        nx = len(crossing)
        pieces = [1] * (total - 2) + [depth] * 2
        first_z, relays = FIRST_Z, RELAYS
        factor = 1.0 / float(tokens * reps) ** 0.5
        dma = lambda n: pltpu.SemaphoreType.DMA((n,))
        vm = pltpu.VMEM
        results = pl.pallas_call(
            functools.partial(kernel, depth, near, far, crossing, marks, first_z, pieces, relays, ORDER, factor),
            out_shape=[
                pltpu.VMEM((tokens, hid), BF16),
                pltpu.VMEM((block, width), F32),
            ],
            in_specs=[pl.BlockSpec(memory_space=pl.ANY)] * 3,
            out_specs=[pl.BlockSpec(memory_space=pltpu.VMEM)] * 2,
            scratch_shapes=[
                vm((tokens, hid), BF16),
                vm((2 * depth, tokens, block), BF16),
                vm((2 * depth * block, 2 * tokens), BF16),
                vm(down_weight.shape, BF16),
                vm((2, 2 * tokens, half), BF16),
                vm((tokens, hid), F32),
                vm((depth, block, width), BF16),
                vm((depth, block, width), BF16),
                vm((depth, block, width), F32),
                vm((depth, block, width), BF16),
                vm((depth, block, width), BF16),
                vm((block, near[0][1]), F32),
                vm((block, near[0][1]), BF16),
                vm((depth, block, far[-1][1]), F32),
                pltpu.SemaphoreType.REGULAR, dma(3), dma(8), dma(2), dma(nn), dma(nx), dma(nx),
                dma(sum(pieces)), dma(1 + total), dma(2),
            ],
            compiler_params=pltpu.CompilerParams(
                collective_id=0, has_side_effects=True, vmem_limit_bytes=56 * 1024 * 1024
            ),
            cost_estimate=pl.CostEstimate(
                flops=8 * tokens * hid * width // 2, bytes_accessed=40 * 1024 * 1024, transcendentals=0),
        )(pre_act, down_weight, cotangent)
        return pl.pallas_call(
            store,
            out_shape=[
                jax.ShapeDtypeStruct((tokens, hid), BF16),
                jax.ShapeDtypeStruct((block, width), F32),
            ],
            in_specs=[pl.BlockSpec(memory_space=pl.ANY)] * 2,
            out_specs=[pl.BlockSpec(memory_space=pl.ANY)] * 2,
            scratch_shapes=[dma(PARTS + 1)],
            compiler_params=pltpu.CompilerParams(vmem_limit_bytes=1024 * 1024),
            cost_estimate=pl.CostEstimate(flops=1, bytes_accessed=10 * 1024 * 1024, transcendentals=0),
        )(*results)

    return jax.shard_map(
        on_device,
        mesh=mesh,
        in_specs=(P("rep", ("fs", "tp")), P(("fs", "tp"), None), P("rep", ("fs", "tp"))),
        out_specs=(P("rep", ("fs", "tp")), P(("fs", "tp", "rep"), None)),
        check_vma=False,
    )
```
